512 devices in a mesh: sp: 16 (over z), dp: 32 (over y, x, core).
Axes of the slice: x: 4, y: 4, z: 16, core: 2. Of those that a mesh axis runs over, the one named last changes fastest.
Arguments:
- up_pre: bfloat16 [32, 6144, 2048], P('dp', 'sp'), may hold values from -6 to 6
- mix_pre: bfloat16 [32, 6144, 2048], P('dp', 'sp'), may hold values from -6 to 6
- ln_gain: float32 [2048], replicated, may hold values from 0.1 to 1.9
- mix_weight: bfloat16 [16, 128, 128], replicated, may hold values from -0.5 to 0.5
- mix_bias: float32 [16, 128], replicated, may hold values from 0.1 to 1.9
- out_weight: bfloat16 [2048, 2048], P('sp', 'dp'), may hold values from -0.125 to 0.125
Outputs:
- mixed_out: bfloat16 [32, 6144, 2048], P('dp', 'sp')
The draws below stay inside these ranges and needn't reach their ends.
All inputs are finite; a program needn't handle non-finite values.
Results may differ from the reference program's by a relative error of at most 0.012.
Values may be sent and summed in bfloat16 or wider, within the bound.
No kernel may reach another device: no remote copies, remote signals or barrier semaphores. Data moves between devices by JAX's collectives and lax.ppermute only.
A program may use at most 64 MiB of HBM per device.

```python
import jax
import jax.numpy as jnp
from jax import lax

D = 2048
E = 2048
GROUPS = 16
BLOCK = 128
SEQS = 32
LENGTH = 6144


def level_of(key, extent, cuts, least, top_value):
    def one(dim, blocks):
        heights = jax.random.uniform(jax.random.fold_in(jax.random.fold_in(key, 6), dim), (blocks,), jnp.float32, least / len(cuts), top_value / len(cuts))
        return jnp.repeat(jnp.exp(heights), extent[dim] // blocks).reshape((-1,) + (1,) * (len(extent) - dim - 1))

    factor_of = one(*cuts[0])
    for cut in cuts[1:]:
        factor_of = factor_of * one(*cut)
    return factor_of


def noise(own_key, extent, scale, reach, cuts=(), kind=jnp.bfloat16):
    loudness = level_of(own_key, extent, cuts, -0.22, 0.18) if cuts else 1.0
    entries = jax.random.normal(own_key, extent, jnp.float32) * scale * loudness
    return jnp.minimum(jnp.maximum(entries, -reach), reach).astype(kind)


def setup_inputs(seed: int = 0) -> dict:
    seeds = jax.random.split(jax.random.key(seed), 7)
    return {
        "up_pre": noise(seeds[0], (SEQS, LENGTH, E), 1.0, 6.0, ((0, 32), (1, 16))),
        "mix_pre": noise(seeds[1], (SEQS, LENGTH, E), 1.0, 6.0, ((0, 32), (1, 16))),
        "ln_gain": jnp.clip(1.0 + 0.18 * jax.random.normal(seeds[2], (E,), jnp.float32), 0.1, 1.9),
        "mix_weight": noise(seeds[3], (GROUPS, BLOCK, BLOCK), BLOCK ** -0.5, 0.5),
        "mix_bias": jnp.clip(1.0 + 0.18 * jax.random.normal(seeds[4], (GROUPS, BLOCK), jnp.float32), 0.1, 1.9),
        "out_weight": noise(seeds[5], (E, D), E ** -0.5, 0.125, ((0, 16), (1, 32))),
    }


norm_epsilon = 1e-05

def one_sequence(operands):
    up_seq, mix_seq, ln_gain, masked, mix_bias, out_weight = operands
    up_act = jax.nn.gelu(up_seq.astype(jnp.float32), approximate=False).astype(jnp.bfloat16)
    activated = jax.nn.gelu(mix_seq.astype(jnp.float32), approximate=False)
    center = lax.optimization_barrier(jnp.mean(activated, axis=-1, keepdims=True))
    spread = lax.optimization_barrier(jnp.mean(jnp.square(activated - center), axis=-1, keepdims=True))
    normed = ((activated - center) * lax.rsqrt(spread + norm_epsilon) * ln_gain).astype(jnp.bfloat16)
    row_count, channels = normed.shape
    blocks = normed.astype(jnp.float32).reshape(row_count // BLOCK, BLOCK, GROUPS, channels // GROUPS)
    mixed_sum = jnp.einsum('gts,nsgc->ntgc', masked, blocks)
    mixed_sum = mixed_sum + jnp.transpose(mix_bias)[None, :, :, None]
    gated = (up_act.astype(jnp.float32) * mixed_sum.reshape(row_count, channels)).astype(jnp.bfloat16)
    return jnp.dot(gated, out_weight, preferred_element_type=jnp.float32).astype(jnp.bfloat16)

def reference(up_pre, mix_pre, ln_gain, mix_weight, mix_bias, out_weight):
    positions = jnp.arange(BLOCK, dtype=jnp.int32)
    causal = positions[:, None] >= positions[None, :]
    masked = jnp.where(causal[None], mix_weight.astype(jnp.float32), jnp.float32(0.0))

    def apply_one(pair):
        return one_sequence((pair[0], pair[1], ln_gain, masked, mix_bias, out_weight))
    return lax.map(apply_one, (up_pre, mix_pre))
```

```python
import functools

import jax
import jax.numpy as jnp
from jax import lax
from jax.experimental import pallas as pl
from jax.experimental.pallas import tpu as pltpu
from jax.sharding import PartitionSpec as P

BLOCK = 128
norm_epsilon = 1e-05
HALF_ROOT = 0.7071067811865476
BF = jnp.bfloat16
F32 = jnp.float32


def gelu(x):
    return (0.5 * x) * (1.0 + lax.erf(x * HALF_ROOT))


def norm_kernel(mix_ref, gain_ref, out_ref, act_ref):
    rows, width = mix_ref.shape
    step = 16

    def body(i, _):
        at = pl.ds(pl.multiple_of(i * step, step), step)
        act = gelu(mix_ref[at, :].astype(F32))
        act_ref[at, :] = act
        center = jnp.sum(act, axis=-1, keepdims=True) * (1.0 / width)
        off = act - center
        spread = jnp.sum(off * off, axis=-1, keepdims=True) * (1.0 / width)
        scale = lax.rsqrt(spread + norm_epsilon)
        out_ref[at, :] = ((act_ref[at, :] - center) * scale * gain_ref[...]).astype(BF)
        return 0

    lax.fori_loop(0, rows // step, body, 0, unroll=2)


def norm(mix, gain):
    rows, width = mix.shape
    return pl.pallas_call(
        norm_kernel,
        grid=(rows // BLOCK,),
        in_specs=[
            pl.BlockSpec((BLOCK, width), lambda i: (i, 0)),
            pl.BlockSpec((1, width), lambda i: (0, 0)),
        ],
        out_specs=pl.BlockSpec((BLOCK, width), lambda i: (i, 0)),
        out_shape=jax.ShapeDtypeStruct((rows, width), BF),
        scratch_shapes=[pltpu.VMEM((BLOCK, width), F32)],
        compiler_params=pltpu.CompilerParams(vmem_limit_bytes=8 << 20),
        cost_estimate=pl.CostEstimate(
            flops=4_000_000_000, bytes_accessed=rows * width * 4, transcendentals=rows * width
        ),
        name="norm",
    )(mix, gain)


def gate_kernel(normed_ref, up_ref, weight_ref, bias_ref, out_ref):
    groups, block, _ = weight_ref.shape
    width = up_ref.shape[1] // groups
    keep = lax.broadcasted_iota(jnp.int32, (block, block), 0) >= lax.broadcasted_iota(
        jnp.int32, (block, block), 1
    )
    for g in range(groups):
        cols = slice(g * width, (g + 1) * width)
        masked = jnp.where(keep, weight_ref[g].astype(F32), 0.0).astype(BF)
        mixed = jnp.dot(masked, normed_ref[:, cols], preferred_element_type=F32)
        mixed = mixed + bias_ref[:, g : g + 1]
        up = gelu(up_ref[:, cols].astype(F32)).astype(BF).astype(F32)
        out_ref[:, cols] = (up * mixed).astype(BF)


def gate(normed, up, weight, bias_t):
    rows, width = up.shape
    groups = weight.shape[0]
    return pl.pallas_call(
        gate_kernel,
        grid=(rows // BLOCK,),
        in_specs=[
            pl.BlockSpec((BLOCK, width), lambda i: (i, 0)),
            pl.BlockSpec((BLOCK, width), lambda i: (i, 0)),
            pl.BlockSpec((groups, BLOCK, BLOCK), lambda i: (0, 0, 0)),
            pl.BlockSpec((BLOCK, groups), lambda i: (0, 0)),
        ],
        out_specs=pl.BlockSpec((BLOCK, width), lambda i: (i, 0)),
        out_shape=jax.ShapeDtypeStruct((rows, width), BF),
        compiler_params=pltpu.CompilerParams(vmem_limit_bytes=8 << 20),
        cost_estimate=pl.CostEstimate(
            flops=4_000_000_000, bytes_accessed=rows * width * 6, transcendentals=rows * width
        ),
        name="gate",
    )(normed, up, weight, bias_t)


def project_kernel(gated_ref, *refs):
    own, other, out_ref = refs[:5], refs[5:10], refs[10]
    index = lax.axis_index("dp")
    core, x, y = index & 1, (index >> 1) & 3, index >> 3
    first, second = lax.select(core == 0, x, y), lax.select(core == 0, y, x)
    blocks = own[0].shape[1]
    half = blocks // 2
    pair = 2 * own[0].shape[2]

    def tile(refs, r, j, k):
        if r == 2:
            return refs[3][j, k] if k < half else refs[4][j, k - half]
        return refs[(0, 1, None, 2)[r]][j, k]

    for r in range(4):
        a = lax.rem(first + r, 4)
        for s in range(0, 4, 2):
            rhs = []
            at = []
            for t in (s, s + 1):
                b = lax.rem(second + t, 4)
                at.append(lax.select(core == 0, b * 4 + a, a * 4 + b))
                rhs.append([tile(own, r, b, k) for k in range(blocks)])
                rhs.append([tile(other, t, a, k) for k in range(blocks)])
            whole = jnp.concatenate([jnp.concatenate(x, axis=1) for x in rhs], axis=0)
            result = lax.dot_general(
                gated_ref[...], whole, (((1,), (1,)), ((), ())), preferred_element_type=F32
            )
            for n in range(2):
                part = pltpu.roll(result[:, n * pair : (n + 1) * pair], core * (pair // 2), 1)
                where = pl.ds(pl.multiple_of(at[n] * pair, pair), pair)
                out_ref[:, where] = part.astype(BF)


def project(gated, own, other):
    rows = gated.shape[0]
    width = 16 * 2 * own[0].shape[2]
    vmem = pl.BlockSpec(memory_space=pltpu.VMEM)
    return pl.pallas_call(
        project_kernel,
        in_specs=[vmem] * 11,
        out_specs=vmem,
        out_shape=jax.ShapeDtypeStruct((rows, width), BF),
        compiler_params=pltpu.CompilerParams(vmem_limit_bytes=6 << 20),
        cost_estimate=pl.CostEstimate(
            flops=2 * rows * width * gated.shape[1], bytes_accessed=12 << 20, transcendentals=0
        ),
        name="project",
    )(gated, *own, *other)


def at(y, x, core):
    return (y % 4 * 4 + x % 4) * 2 + core


GROUPS = [[at(y, x, 0) for y in range(4)] for x in range(4)] + [
    [at(y, x, 1) for x in range(4)] for y in range(4)
]


def ring(shift):
    pairs = []
    for y in range(4):
        for x in range(4):
            pairs.append((at(y, x, 0), at(y, x + shift, 0)))
            pairs.append((at(y, x, 1), at(y + shift, x, 1)))
    return pairs


SWAP = [(d, d ^ 1) for d in range(32)]


def sent_to_all(value, axis, length, groups=None):
    return lax.all_to_all(
        jnp.broadcast_to(value[None], (length, *value.shape)),
        axis,
        0,
        0,
        tiled=True,
        axis_index_groups=groups,
    )


def per_device(up_pre, mix_pre, ln_gain, mix_weight, mix_bias, out_weight):
    slab = sent_to_all(out_weight.T, "sp", 16)
    normed = norm(mix_pre[0], ln_gain[None])
    slab, normed = lax.optimization_barrier((slab, normed))
    own = sent_to_all(slab, "dp", 4, GROUPS)
    gated = gate(normed, up_pre[0], mix_weight, mix_bias.T)
    own, gated = lax.optimization_barrier((own, gated))
    before = lax.ppermute(own, "dp", ring(1))
    after = lax.ppermute(own, "dp", ring(-1))
    other = lax.ppermute(own, "dp", SWAP)
    before, after, other = lax.optimization_barrier((before, after, other))
    far_low = lax.ppermute(before[:, :8], "dp", ring(1))
    far_high = lax.ppermute(after[:, 8:], "dp", ring(-1))
    mine = [own, after, before, far_low, far_high]
    theirs = [other] + [lax.ppermute(v, "dp", SWAP) for v in mine[1:]]
    return project(gated, mine, theirs)[None]


def solution(mesh):
    return jax.shard_map(
        per_device,
        mesh=mesh,
        in_specs=(P("dp", "sp", None), P("dp", "sp", None), P(), P(), P(), P("sp", "dp")),
        out_specs=P("dp", "sp", None),
        check_vma=False,
    )
```

```python
import jax
import jax.numpy as jnp
from jax import lax
from jax.experimental import pallas as pl
from jax.experimental.pallas import tpu as pltpu
from jax.sharding import PartitionSpec as P


BLOCK = 128
norm_epsilon = 1e-05
HALF_ROOT = 0.7071067811865476
BF = jnp.bfloat16
F32 = jnp.float32


def gelu(x):
    return (0.5 * x) * (1.0 + lax.erf(x * HALF_ROOT))


def norm_kernel(mix_ref, gain_ref, out_ref, act_ref):
    rows, width = mix_ref.shape
    step = 16

    def body(i, _):
        at = pl.ds(pl.multiple_of(i * step, step), step)
        act = gelu(mix_ref[at, :].astype(F32))
        act_ref[at, :] = act
        center = jnp.sum(act, axis=-1, keepdims=True) * (1.0 / width)
        off = act - center
        spread = jnp.sum(off * off, axis=-1, keepdims=True) * (1.0 / width)
        scale = lax.rsqrt(spread + norm_epsilon)
        out_ref[at, :] = ((act_ref[at, :] - center) * scale * gain_ref[...]).astype(BF)
        return 0

    lax.fori_loop(0, rows // step, body, 0, unroll=2)


def norm(mix, gain):
    rows, width = mix.shape
    return pl.pallas_call(
        norm_kernel,
        grid=(rows // BLOCK,),
        in_specs=[
            pl.BlockSpec((BLOCK, width), lambda i: (i, 0)),
            pl.BlockSpec((1, width), lambda i: (0, 0)),
        ],
        out_specs=pl.BlockSpec((BLOCK, width), lambda i: (i, 0)),
        out_shape=jax.ShapeDtypeStruct((rows, width), BF),
        scratch_shapes=[pltpu.VMEM((BLOCK, width), F32)],
        compiler_params=pltpu.CompilerParams(vmem_limit_bytes=8 << 20),
        cost_estimate=pl.CostEstimate(
            flops=4_000_000_000, bytes_accessed=rows * width * 4, transcendentals=rows * width
        ),
        name="norm",
    )(mix, gain)


def gate_kernel(normed_ref, up_ref, weight_ref, bias_ref, out_ref):
    groups, block, _ = weight_ref.shape
    width = up_ref.shape[1] // groups
    keep = lax.broadcasted_iota(jnp.int32, (block, block), 0) >= lax.broadcasted_iota(
        jnp.int32, (block, block), 1
    )
    bias = jnp.transpose(bias_ref[...])
    for g in range(groups):
        cols = slice(g * width, (g + 1) * width)
        masked = jnp.where(keep, weight_ref[g].astype(F32), 0.0).astype(BF)
        mixed = jnp.dot(masked, normed_ref[:, cols], preferred_element_type=F32)
        mixed = mixed + bias[:, g : g + 1]
        up = gelu(up_ref[:, cols].astype(F32)).astype(BF).astype(F32)
        out_ref[:, cols] = (up * mixed).astype(BF)


def gate(normed, up, weight, bias):
    rows, width = up.shape
    groups = weight.shape[0]
    return pl.pallas_call(
        gate_kernel,
        grid=(rows // BLOCK,),
        in_specs=[
            pl.BlockSpec((BLOCK, width), lambda i: (i, 0)),
            pl.BlockSpec((BLOCK, width), lambda i: (i, 0)),
            pl.BlockSpec((groups, BLOCK, BLOCK), lambda i: (0, 0, 0)),
            pl.BlockSpec((groups, BLOCK), lambda i: (0, 0)),
        ],
        out_specs=pl.BlockSpec((BLOCK, width), lambda i: (i, 0)),
        out_shape=jax.ShapeDtypeStruct((rows, width), BF),
        compiler_params=pltpu.CompilerParams(vmem_limit_bytes=8 << 20),
        cost_estimate=pl.CostEstimate(
            flops=4_000_000_000, bytes_accessed=rows * width * 6, transcendentals=rows * width
        ),
        name="gate",
    )(normed, up, weight, bias)


def project_kernel(gated_ref, *refs):
    pieces, out_ref = refs[:-1], refs[-1]
    index = lax.axis_index("dp")
    core, x, y = index & 1, (index >> 1) & 3, index >> 3
    first, second = lax.select(core == 0, x, y), lax.select(core == 0, y, x)
    own, low1, high1, low2, high2, low3, high3, other, near, far = pieces
    blocks = own.shape[1]
    half = blocks // 2
    pair = 2 * own.shape[2]

    def mine(r, j, k):
        if r == 0:
            return own[j, k]
        low, high = ((low1, high1), (low2, high2), (low3, high3))[r - 1]
        return low[j, k] if k < half else high[j, k - half]

    def theirs(r, j, k):
        if r == 0:
            return other[j, k]
        part = k // half
        if r == 2:
            return far[part, j, k % half]
        return near[(r - 1) + part, j, k % half]

    for r in range(4):
        a = lax.rem(first + r, 4)
        for s in range(0, 4, 2):
            rhs = []
            at = []
            for t in (s, s + 1):
                b = lax.rem(second + t, 4)
                at.append(lax.select(core == 0, b * 4 + a, a * 4 + b))
                rhs.append([mine(r, b, k) for k in range(blocks)])
                rhs.append([theirs(t, a, k) for k in range(blocks)])
            whole = jnp.concatenate([jnp.concatenate(x, axis=1) for x in rhs], axis=0)
            result = lax.dot_general(
                gated_ref[...], whole, (((1,), (1,)), ((), ())), preferred_element_type=F32
            )
            for n in range(2):
                part = pltpu.roll(result[:, n * pair : (n + 1) * pair], core * (pair // 2), 1)
                where = pl.ds(pl.multiple_of(at[n] * pair, pair), pair)
                out_ref[:, where] = part.astype(BF)


def project(gated, pieces):
    rows = gated.shape[0]
    width = 16 * 2 * pieces[0].shape[2]
    vmem = pl.BlockSpec(memory_space=pltpu.VMEM)
    return pl.pallas_call(
        project_kernel,
        in_specs=[vmem] * (1 + len(pieces)),
        out_specs=vmem,
        out_shape=jax.ShapeDtypeStruct((rows, width), BF),
        compiler_params=pltpu.CompilerParams(vmem_limit_bytes=6 << 20),
        cost_estimate=pl.CostEstimate(
            flops=2 * rows * width * gated.shape[1], bytes_accessed=12 << 20, transcendentals=0
        ),
        name="project",
    )(gated, *pieces)


def at(y, x, core):
    return (y % 4 * 4 + x % 4) * 2 + core


GROUPS = [[at(y, x, 0) for y in range(4)] for x in range(4)] + [
    [at(y, x, 1) for x in range(4)] for y in range(4)
]


def ring(shift):
    pairs = []
    for y in range(4):
        for x in range(4):
            pairs.append((at(y, x, 0), at(y, x + shift, 0)))
            pairs.append((at(y, x, 1), at(y + shift, x, 1)))
    return pairs


SWAP = [(d, d ^ 1) for d in range(32)]


def sent_to_all(value, axis, length, groups=None):
    return lax.all_to_all(
        jnp.broadcast_to(value[None], (length, *value.shape)),
        axis,
        0,
        0,
        tiled=True,
        axis_index_groups=groups,
    )


def moved(value, pairs):
    return lax.ppermute(value, "dp", pairs)


def per_device(up_pre, mix_pre, ln_gain, mix_weight, mix_bias, out_weight):
    slab = sent_to_all(out_weight.T, "sp", 16)
    own = sent_to_all(slab, "dp", 4, GROUPS)
    low, high = own[:, :8], own[:, 8:]
    low3 = moved(low, ring(1))
    high1 = moved(high, ring(-1))
    high3 = moved(high, ring(1))
    low1 = moved(low, ring(-1))
    low3, high1, ln_gain = lax.optimization_barrier((low3, high1, ln_gain))
    low2 = moved(low3, ring(1))
    high2 = moved(high1, ring(-1))
    other = moved(own, SWAP)
    normed = norm(mix_pre[0], ln_gain[None])
    low1, high3, normed = lax.optimization_barrier((low1, high3, normed))
    near = moved(jnp.stack([low1, high1, low3, high3]), SWAP)
    gated = gate(normed, up_pre[0], mix_weight, mix_bias)
    low2, high2, gated = lax.optimization_barrier((low2, high2, gated))
    far = moved(jnp.stack([low2, high2]), SWAP)
    pieces = [own, low1, high1, low2, high2, low3, high3, other, near, far]
    return project(gated, pieces)[None]


def solution(mesh):
    return jax.shard_map(
        per_device,
        mesh=mesh,
        in_specs=(P("dp", "sp", None), P("dp", "sp", None), P(), P(), P(), P("sp", "dp")),
        out_specs=P("dp", "sp", None),
        check_vma=False,
    )
```

```python
import jax
import jax.numpy as jnp
from jax import lax
from jax.experimental import pallas as pl
from jax.experimental.pallas import tpu as pltpu
from jax.sharding import PartitionSpec as P


BLOCK = 128
norm_epsilon = 1e-05
HALF_ROOT = 0.7071067811865476
BF = jnp.bfloat16
F32 = jnp.float32


def gelu(x):
    return (0.5 * x) * (1.0 + lax.erf(x * HALF_ROOT))


def norm_kernel(mix_ref, gain_ref, out_ref, act_ref):
    rows, width = mix_ref.shape
    step = 16

    def body(i, _):
        at = pl.ds(pl.multiple_of(i * step, step), step)
        act = gelu(mix_ref[at, :].astype(F32))
        act_ref[at, :] = act
        center = jnp.sum(act, axis=-1, keepdims=True) * (1.0 / width)
        off = act - center
        spread = jnp.sum(off * off, axis=-1, keepdims=True) * (1.0 / width)
        scale = lax.rsqrt(spread + norm_epsilon)
        out_ref[at, :] = ((act_ref[at, :] - center) * scale * gain_ref[...]).astype(BF)
        return 0

    lax.fori_loop(0, rows // step, body, 0, unroll=2)


def norm(mix, gain):
    rows, width = mix.shape
    return pl.pallas_call(
        norm_kernel,
        grid=(rows // BLOCK,),
        in_specs=[
            pl.BlockSpec((BLOCK, width), lambda i: (i, 0)),
            pl.BlockSpec((1, width), lambda i: (0, 0)),
        ],
        out_specs=pl.BlockSpec((BLOCK, width), lambda i: (i, 0)),
        out_shape=jax.ShapeDtypeStruct((rows, width), BF),
        scratch_shapes=[pltpu.VMEM((BLOCK, width), F32)],
        compiler_params=pltpu.CompilerParams(vmem_limit_bytes=8 << 20),
        cost_estimate=pl.CostEstimate(
            flops=4_000_000_000, bytes_accessed=rows * width * 4, transcendentals=rows * width
        ),
        name="norm",
    )(mix, gain)


def gate_kernel(normed_ref, up_ref, weight_ref, bias_ref, out_ref):
    groups, block, _ = weight_ref.shape
    width = up_ref.shape[1] // groups
    keep = lax.broadcasted_iota(jnp.int32, (block, block), 0) >= lax.broadcasted_iota(
        jnp.int32, (block, block), 1
    )
    bias = jnp.transpose(bias_ref[...])
    for g in range(groups):
        cols = slice(g * width, (g + 1) * width)
        masked = jnp.where(keep, weight_ref[g].astype(F32), 0.0).astype(BF)
        mixed = jnp.dot(masked, normed_ref[:, cols], preferred_element_type=F32)
        mixed = mixed + bias[:, g : g + 1]
        up = gelu(up_ref[:, cols].astype(F32)).astype(BF).astype(F32)
        out_ref[:, cols] = (up * mixed).astype(BF)


def gate(normed, up, weight, bias):
    rows, width = up.shape
    groups = weight.shape[0]
    return pl.pallas_call(
        gate_kernel,
        grid=(rows // BLOCK,),
        in_specs=[
            pl.BlockSpec((BLOCK, width), lambda i: (i, 0)),
            pl.BlockSpec((BLOCK, width), lambda i: (i, 0)),
            pl.BlockSpec((groups, BLOCK, BLOCK), lambda i: (0, 0, 0)),
            pl.BlockSpec((groups, BLOCK), lambda i: (0, 0)),
        ],
        out_specs=pl.BlockSpec((BLOCK, width), lambda i: (i, 0)),
        out_shape=jax.ShapeDtypeStruct((rows, width), BF),
        compiler_params=pltpu.CompilerParams(vmem_limit_bytes=8 << 20),
        cost_estimate=pl.CostEstimate(
            flops=4_000_000_000, bytes_accessed=rows * width * 6, transcendentals=rows * width
        ),
        name="gate",
    )(normed, up, weight, bias)


def project_kernel(mine_ref, partner_ref, *refs):
    pieces, kept_ref, sent_ref = refs[:-2], refs[-2], refs[-1]
    core = lax.axis_index("dp") & 1
    for n, piece in enumerate(pieces):
        count, blocks, width, _ = piece.shape
        rhs = jnp.concatenate(
            [
                jnp.concatenate([piece[j, k] for k in range(blocks)], axis=1)
                for j in range(count)
            ],
            axis=0,
        )
        for rows_ref, out_ref in ((mine_ref, kept_ref), (partner_ref, sent_ref)):
            result = lax.dot_general(
                rows_ref[...], rhs, (((1,), (1,)), ((), ())), preferred_element_type=F32
            )
            for m in range(count // 2):
                tile = result[:, m * 2 * width : (m + 1) * 2 * width]
                first = n * count + 2 * m
                out_ref[first + core] = tile.astype(BF)
                out_ref[first + 1 - core] = pltpu.roll(tile, width, 1).astype(BF)


def project(mine, partner, pieces):
    rows = mine.shape[0]
    count, _, width, _ = pieces[0].shape
    tiles = len(pieces) * count
    vmem = pl.BlockSpec(memory_space=pltpu.VMEM)
    out = jax.ShapeDtypeStruct((tiles, rows, 2 * width), BF)
    return pl.pallas_call(
        project_kernel,
        in_specs=[vmem] * (2 + len(pieces)),
        out_specs=[vmem, vmem],
        out_shape=[out, out],
        compiler_params=pltpu.CompilerParams(vmem_limit_bytes=6 << 20),
        cost_estimate=pl.CostEstimate(
            flops=4 * rows * width * tiles * mine.shape[1], bytes_accessed=4 << 20, transcendentals=0
        ),
        name="project",
    )(mine, partner, *pieces)


ORDER = (0, 1, 3, 2)


def merge_kernel(kept1, kept2, got1, got2, out_ref):
    index = lax.axis_index("dp")
    core, x, y = index & 1, (index >> 1) & 3, index >> 3
    first, second = lax.select(core == 0, x, y), lax.select(core == 0, y, x)
    step = out_ref.shape[0]
    width = kept1.shape[2]
    rows = pl.ds(pl.multiple_of(pl.program_id(0) * step, step), step)
    lane = lax.broadcasted_iota(jnp.int32, (step, width), 1)
    ours = (lane // (width // 2)) == core

    def tile(refs, r, j):
        place = ORDER.index(r)
        return refs[0][place * 4 + j, rows, :] if place < 3 else refs[1][j, rows, :]

    for r in range(4):
        a = lax.rem(first + r, 4)
        for t in range(4):
            b = lax.rem(second + t, 4)
            at = lax.select(core == 0, b * 4 + a, a * 4 + b)
            kept = tile((kept1, kept2), r, b).astype(F32)
            got = tile((got1, got2), t, a).astype(F32)
            where = pl.ds(pl.multiple_of(at * width, width), width)
            out_ref[:, where] = jnp.where(ours, kept, got).astype(BF)


def merge(kept1, kept2, got1, got2):
    rows, width = kept1.shape[1:]
    vmem = pl.BlockSpec(memory_space=pltpu.VMEM)
    return pl.pallas_call(
        merge_kernel,
        grid=(rows // BLOCK,),
        in_specs=[vmem] * 4,
        out_specs=pl.BlockSpec((BLOCK, 16 * width), lambda i: (i, 0)),
        out_shape=jax.ShapeDtypeStruct((rows, 16 * width), BF),
        compiler_params=pltpu.CompilerParams(vmem_limit_bytes=4 << 20),
        name="merge",
    )(kept1, kept2, got1, got2)


def at(y, x, core):
    return (y % 4 * 4 + x % 4) * 2 + core


GROUPS = [[at(y, x, 0) for y in range(4)] for x in range(4)] + [
    [at(y, x, 1) for x in range(4)] for y in range(4)
]


def ring(shift):
    pairs = []
    for y in range(4):
        for x in range(4):
            pairs.append((at(y, x, 0), at(y, x + shift, 0)))
            pairs.append((at(y, x, 1), at(y + shift, x, 1)))
    return pairs


SWAP = [(d, d ^ 1) for d in range(32)]


def sent_to_all(value, axis, length, groups=None):
    return lax.all_to_all(
        jnp.broadcast_to(value[None], (length, *value.shape)),
        axis,
        0,
        0,
        tiled=True,
        axis_index_groups=groups,
    )


def moved(value, pairs):
    return lax.ppermute(value, "dp", pairs)


def per_device(up_pre, mix_pre, ln_gain, mix_weight, mix_bias, out_weight):
    slab = sent_to_all(out_weight.T, "sp", 16)
    normed = norm(mix_pre[0], ln_gain[None])
    gated = gate(normed, up_pre[0], mix_weight, mix_bias)
    slab, gated = lax.optimization_barrier((slab, gated))
    own = sent_to_all(slab, "dp", 4, GROUPS)
    before = moved(own, ring(1))
    after = moved(own, ring(-1))
    across = moved(own, ring(2))
    partner = moved(gated, SWAP)
    kept1, sent1 = project(gated, partner, [own, after, before])
    across, kept1 = lax.optimization_barrier((across, kept1))
    got1 = moved(sent1, SWAP)
    kept2, sent2 = project(gated, partner, [across])
    got2 = moved(sent2, SWAP)
    return merge(kept1, kept2, got1, got2)[None]


def solution(mesh):
    return jax.shard_map(
        per_device,
        mesh=mesh,
        in_specs=(P("dp", "sp", None), P("dp", "sp", None), P(), P(), P(), P("sp", "dp")),
        out_specs=P("dp", "sp", None),
        check_vma=False,
    )
```

```python
import functools

import jax
import jax.numpy as jnp
from jax import lax
from jax.experimental import pallas as pl
from jax.experimental.pallas import tpu as pltpu
from jax.sharding import PartitionSpec as P


BLOCK = 128
norm_epsilon = 1e-05
HALF_ROOT = 0.7071067811865476
BF = jnp.bfloat16
F32 = jnp.float32


def gelu(x):
    return (0.5 * x) * (1.0 + lax.erf(x * HALF_ROOT))


def norm_kernel(mix_ref, gain_ref, out_ref, act_ref):
    rows, width = mix_ref.shape
    step = 16

    def body(i, _):
        at = pl.ds(pl.multiple_of(i * step, step), step)
        act = gelu(mix_ref[at, :].astype(F32))
        act_ref[at, :] = act
        center = jnp.sum(act, axis=-1, keepdims=True) * (1.0 / width)
        off = act - center
        spread = jnp.sum(off * off, axis=-1, keepdims=True) * (1.0 / width)
        scale = lax.rsqrt(spread + norm_epsilon)
        out_ref[at, :] = ((act_ref[at, :] - center) * scale * gain_ref[...]).astype(BF)
        return 0

    lax.fori_loop(0, rows // step, body, 0, unroll=2)


def norm(mix, gain):
    rows, width = mix.shape
    return pl.pallas_call(
        norm_kernel,
        grid=(rows // BLOCK,),
        in_specs=[
            pl.BlockSpec((BLOCK, width), lambda i: (i, 0)),
            pl.BlockSpec((1, width), lambda i: (0, 0)),
        ],
        out_specs=pl.BlockSpec((BLOCK, width), lambda i: (i, 0)),
        out_shape=jax.ShapeDtypeStruct((rows, width), BF),
        scratch_shapes=[pltpu.VMEM((BLOCK, width), F32)],
        compiler_params=pltpu.CompilerParams(vmem_limit_bytes=8 << 20),
        cost_estimate=pl.CostEstimate(
            flops=4_000_000_000, bytes_accessed=rows * width * 4, transcendentals=rows * width
        ),
        name="norm",
    )(mix, gain)


def gate_kernel(normed_ref, up_ref, weight_ref, bias_ref, out_ref):
    groups, block, _ = weight_ref.shape
    width = up_ref.shape[1] // groups
    keep = lax.broadcasted_iota(jnp.int32, (block, block), 0) >= lax.broadcasted_iota(
        jnp.int32, (block, block), 1
    )
    bias = jnp.transpose(bias_ref[...])
    for g in range(groups):
        cols = slice(g * width, (g + 1) * width)
        masked = jnp.where(keep, weight_ref[g].astype(F32), 0.0).astype(BF)
        mixed = jnp.dot(masked, normed_ref[:, cols], preferred_element_type=F32)
        mixed = mixed + bias[:, g : g + 1]
        up = gelu(up_ref[:, cols].astype(F32)).astype(BF).astype(F32)
        out_ref[:, cols] = (up * mixed).astype(BF)


def gate(normed, up, weight, bias):
    rows, width = up.shape
    groups = weight.shape[0]
    return pl.pallas_call(
        gate_kernel,
        grid=(rows // BLOCK,),
        in_specs=[
            pl.BlockSpec((BLOCK, width), lambda i: (i, 0)),
            pl.BlockSpec((BLOCK, width), lambda i: (i, 0)),
            pl.BlockSpec((groups, BLOCK, BLOCK), lambda i: (0, 0, 0)),
            pl.BlockSpec((groups, BLOCK), lambda i: (0, 0)),
        ],
        out_specs=pl.BlockSpec((BLOCK, width), lambda i: (i, 0)),
        out_shape=jax.ShapeDtypeStruct((rows, width), BF),
        compiler_params=pltpu.CompilerParams(vmem_limit_bytes=8 << 20),
        cost_estimate=pl.CostEstimate(
            flops=4_000_000_000, bytes_accessed=rows * width * 6, transcendentals=rows * width
        ),
        name="gate",
    )(normed, up, weight, bias)


def project_kernel(split, mine_ref, partner_ref, *refs):
    parts, kept_ref, sent_ref = refs[:-2], refs[-2], refs[-1]
    core = lax.axis_index("dp") & 1
    for n in range(len(parts) // split):
        piece = parts[n * split : (n + 1) * split]
        count, blocks, width, _ = piece[0].shape
        rhs = jnp.concatenate(
            [
                jnp.concatenate([p[j, k] for p in piece for k in range(blocks)], axis=1)
                for j in range(count)
            ],
            axis=0,
        )
        for rows_ref, out_ref in ((mine_ref, kept_ref), (partner_ref, sent_ref)):
            result = lax.dot_general(
                rows_ref[...], rhs, (((1,), (1,)), ((), ())), preferred_element_type=F32
            )
            for m in range(count // 2):
                tile = result[:, m * 2 * width : (m + 1) * 2 * width]
                first = n * count + 2 * m
                out_ref[first + core] = tile.astype(BF)
                out_ref[first + 1 - core] = pltpu.roll(tile, width, 1).astype(BF)


def project(mine, partner, parts, split):
    rows = mine.shape[0]
    count, _, width, _ = parts[0].shape
    tiles = len(parts) // split * count
    vmem = pl.BlockSpec(memory_space=pltpu.VMEM)
    out = jax.ShapeDtypeStruct((tiles, rows, 2 * width), BF)
    return pl.pallas_call(
        functools.partial(project_kernel, split),
        in_specs=[vmem] * (2 + len(parts)),
        out_specs=[vmem, vmem],
        out_shape=[out, out],
        compiler_params=pltpu.CompilerParams(vmem_limit_bytes=6 << 20),
        cost_estimate=pl.CostEstimate(
            flops=4 * rows * width * tiles * mine.shape[1], bytes_accessed=4 << 20, transcendentals=0
        ),
        name="project",
    )(mine, partner, *parts)


ORDER = (0, 1, 3, 2)


def merge_kernel(kept1, kept2, got1, got2, out_ref):
    index = lax.axis_index("dp")
    core, x, y = index & 1, (index >> 1) & 3, index >> 3
    first, second = lax.select(core == 0, x, y), lax.select(core == 0, y, x)
    step = out_ref.shape[0]
    width = kept1.shape[2]
    rows = pl.ds(pl.multiple_of(pl.program_id(0) * step, step), step)
    lane = lax.broadcasted_iota(jnp.int32, (step, width), 1)
    ours = (lane // (width // 2)) == core

    def tile(refs, r, j):
        place = ORDER.index(r)
        return refs[0][place * 4 + j, rows, :] if place < 3 else refs[1][j, rows, :]

    for r in range(4):
        a = lax.rem(first + r, 4)
        for t in range(4):
            b = lax.rem(second + t, 4)
            at = lax.select(core == 0, b * 4 + a, a * 4 + b)
            kept = tile((kept1, kept2), r, b).astype(F32)
            got = tile((got1, got2), t, a).astype(F32)
            where = pl.ds(pl.multiple_of(at * width, width), width)
            out_ref[:, where] = jnp.where(ours, kept, got).astype(BF)


def merge(kept1, kept2, got1, got2):
    rows, width = kept1.shape[1:]
    vmem = pl.BlockSpec(memory_space=pltpu.VMEM)
    return pl.pallas_call(
        merge_kernel,
        grid=(rows // BLOCK,),
        in_specs=[vmem] * 4,
        out_specs=pl.BlockSpec((BLOCK, 16 * width), lambda i: (i, 0)),
        out_shape=jax.ShapeDtypeStruct((rows, 16 * width), BF),
        compiler_params=pltpu.CompilerParams(vmem_limit_bytes=4 << 20),
        name="merge",
    )(kept1, kept2, got1, got2)


def at(y, x, core):
    return (y % 4 * 4 + x % 4) * 2 + core


GROUPS = [[at(y, x, 0) for y in range(4)] for x in range(4)] + [
    [at(y, x, 1) for x in range(4)] for y in range(4)
]


def ring(shift):
    pairs = []
    for y in range(4):
        for x in range(4):
            pairs.append((at(y, x, 0), at(y, x + shift, 0)))
            pairs.append((at(y, x, 1), at(y + shift, x, 1)))
    return pairs


SWAP = [(d, d ^ 1) for d in range(32)]


def sent_to_all(value, axis, length, groups=None):
    return lax.all_to_all(
        jnp.broadcast_to(value[None], (length, *value.shape)),
        axis,
        0,
        0,
        tiled=True,
        axis_index_groups=groups,
    )


def moved(value, pairs):
    return lax.ppermute(value, "dp", pairs)


def per_device(up_pre, mix_pre, ln_gain, mix_weight, mix_bias, out_weight):
    slab = sent_to_all(out_weight.T, "sp", 16)
    normed = norm(mix_pre[0], ln_gain[None])
    gated = gate(normed, up_pre[0], mix_weight, mix_bias)
    partner = moved(gated, SWAP)
    slab, partner = lax.optimization_barrier((slab, partner))
    own = sent_to_all(slab, "dp", 4, GROUPS)
    before = moved(own, ring(1))
    after = moved(own, ring(-1))
    low2 = moved(before[:, :8], ring(1))
    high2 = moved(after[:, 8:], ring(-1))
    kept1, sent1 = project(gated, partner, [own, after, before], 1)
    got1 = moved(sent1, SWAP)
    low2, high2, kept1 = lax.optimization_barrier((low2, high2, kept1))
    kept2, sent2 = project(gated, partner, [low2, high2], 2)
    got2 = moved(sent2, SWAP)
    return merge(kept1, kept2, got1, got2)[None]


def solution(mesh):
    return jax.shard_map(
        per_device,
        mesh=mesh,
        in_specs=(P("dp", "sp", None), P("dp", "sp", None), P(), P(), P(), P("sp", "dp")),
        out_specs=P("dp", "sp", None),
        check_vma=False,
    )
```

```python
import functools

import jax
import jax.numpy as jnp
from jax import lax
from jax.experimental import pallas as pl
from jax.experimental.pallas import tpu as pltpu
from jax.sharding import PartitionSpec as P


BLOCK = 128
norm_epsilon = 1e-05
HALF_ROOT = 0.7071067811865476
BF = jnp.bfloat16
F32 = jnp.float32


def gelu(x):
    return (0.5 * x) * (1.0 + lax.erf(x * HALF_ROOT))


def norm_kernel(mix_ref, gain_ref, out_ref, act_ref):
    rows, width = mix_ref.shape
    step = 16

    def body(i, _):
        at = pl.ds(pl.multiple_of(i * step, step), step)
        act = gelu(mix_ref[at, :].astype(F32))
        act_ref[at, :] = act
        center = jnp.sum(act, axis=-1, keepdims=True) * (1.0 / width)
        off = act - center
        spread = jnp.sum(off * off, axis=-1, keepdims=True) * (1.0 / width)
        scale = lax.rsqrt(spread + norm_epsilon)
        out_ref[at, :] = ((act_ref[at, :] - center) * scale * gain_ref[...]).astype(BF)
        return 0

    lax.fori_loop(0, rows // step, body, 0, unroll=2)


def norm(mix, gain):
    rows, width = mix.shape
    return pl.pallas_call(
        norm_kernel,
        grid=(rows // BLOCK,),
        in_specs=[
            pl.BlockSpec((BLOCK, width), lambda i: (i, 0)),
            pl.BlockSpec((1, width), lambda i: (0, 0)),
        ],
        out_specs=pl.BlockSpec((BLOCK, width), lambda i: (i, 0)),
        out_shape=jax.ShapeDtypeStruct((rows, width), BF),
        scratch_shapes=[pltpu.VMEM((BLOCK, width), F32)],
        compiler_params=pltpu.CompilerParams(vmem_limit_bytes=8 << 20),
        cost_estimate=pl.CostEstimate(
            flops=4_000_000_000, bytes_accessed=rows * width * 4, transcendentals=rows * width
        ),
        name="norm",
    )(mix, gain)


def gate_kernel(normed_ref, up_ref, weight_ref, bias_ref, out_ref):
    groups, block, _ = weight_ref.shape
    width = up_ref.shape[1] // groups
    keep = lax.broadcasted_iota(jnp.int32, (block, block), 0) >= lax.broadcasted_iota(
        jnp.int32, (block, block), 1
    )
    bias = jnp.transpose(bias_ref[...])
    for g in range(groups):
        cols = slice(g * width, (g + 1) * width)
        masked = jnp.where(keep, weight_ref[g].astype(F32), 0.0).astype(BF)
        mixed = jnp.dot(masked, normed_ref[:, cols], preferred_element_type=F32)
        mixed = mixed + bias[:, g : g + 1]
        up = gelu(up_ref[:, cols].astype(F32)).astype(BF).astype(F32)
        out_ref[:, cols] = (up * mixed).astype(BF)


def gate(normed, up, weight, bias):
    rows, width = up.shape
    groups = weight.shape[0]
    return pl.pallas_call(
        gate_kernel,
        grid=(rows // BLOCK,),
        in_specs=[
            pl.BlockSpec((BLOCK, width), lambda i: (i, 0)),
            pl.BlockSpec((BLOCK, width), lambda i: (i, 0)),
            pl.BlockSpec((groups, BLOCK, BLOCK), lambda i: (0, 0, 0)),
            pl.BlockSpec((groups, BLOCK), lambda i: (0, 0)),
        ],
        out_specs=pl.BlockSpec((BLOCK, width), lambda i: (i, 0)),
        out_shape=jax.ShapeDtypeStruct((rows, width), BF),
        compiler_params=pltpu.CompilerParams(vmem_limit_bytes=8 << 20),
        cost_estimate=pl.CostEstimate(
            flops=4_000_000_000, bytes_accessed=rows * width * 6, transcendentals=rows * width
        ),
        name="gate",
    )(normed, up, weight, bias)


def project_kernel(split, mine_ref, partner_ref, *refs):
    parts, kept_ref, sent_ref = refs[:-2], refs[-2], refs[-1]
    core = lax.axis_index("dp") & 1
    for n, (start, stop) in enumerate(zip(split, split[1:])):
        piece = parts[start:stop]
        count, blocks, width, _ = piece[0].shape
        rhs = jnp.concatenate(
            [
                jnp.concatenate([p[j, k] for p in piece for k in range(blocks)], axis=1)
                for j in range(count)
            ],
            axis=0,
        )
        for rows_ref, out_ref in ((mine_ref, kept_ref), (partner_ref, sent_ref)):
            result = lax.dot_general(
                rows_ref[...], rhs, (((1,), (1,)), ((), ())), preferred_element_type=F32
            )
            for m in range(count // 2):
                tile = result[:, m * 2 * width : (m + 1) * 2 * width]
                first = n * count + 2 * m
                out_ref[first + core] = tile.astype(BF)
                out_ref[first + 1 - core] = pltpu.roll(tile, width, 1).astype(BF)


def project(mine, partner, pieces):
    rows = mine.shape[0]
    count, _, width, _ = pieces[0][0].shape
    tiles = len(pieces) * count
    parts = [part for piece in pieces for part in piece]
    split = [sum(len(piece) for piece in pieces[:n]) for n in range(len(pieces) + 1)]
    vmem = pl.BlockSpec(memory_space=pltpu.VMEM)
    out = jax.ShapeDtypeStruct((tiles, rows, 2 * width), BF)
    return pl.pallas_call(
        functools.partial(project_kernel, split),
        in_specs=[vmem] * (2 + len(parts)),
        out_specs=[vmem, vmem],
        out_shape=[out, out],
        compiler_params=pltpu.CompilerParams(vmem_limit_bytes=6 << 20),
        cost_estimate=pl.CostEstimate(
            flops=4 * rows * width * tiles * mine.shape[1], bytes_accessed=4 << 20, transcendentals=0
        ),
        name="project",
    )(mine, partner, *parts)


ORDER = (0, 1, 3, 2)


def merge_kernel(kept1, kept2, got1, got2, out_ref):
    index = lax.axis_index("dp")
    core, x, y = index & 1, (index >> 1) & 3, index >> 3
    first, second = lax.select(core == 0, x, y), lax.select(core == 0, y, x)
    step = out_ref.shape[0]
    width = kept1.shape[2]
    rows = pl.ds(pl.multiple_of(pl.program_id(0) * step, step), step)
    lane = lax.broadcasted_iota(jnp.int32, (step, width), 1)
    ours = (lane // (width // 2)) == core

    def tile(refs, r, j):
        place = ORDER.index(r)
        return refs[0][place * 4 + j, rows, :] if place < 3 else refs[1][j, rows, :]

    for r in range(4):
        a = lax.rem(first + r, 4)
        for t in range(4):
            b = lax.rem(second + t, 4)
            at = lax.select(core == 0, b * 4 + a, a * 4 + b)
            kept = tile((kept1, kept2), r, b)
            got = tile((got1, got2), t, a)
            where = pl.ds(pl.multiple_of(at * width, width), width)
            out_ref[:, where] = jnp.where(ours, kept, got)


def merge(kept1, kept2, got1, got2):
    rows, width = kept1.shape[1:]
    vmem = pl.BlockSpec(memory_space=pltpu.VMEM)
    return pl.pallas_call(
        merge_kernel,
        grid=(rows // BLOCK,),
        in_specs=[vmem] * 4,
        out_specs=pl.BlockSpec((BLOCK, 16 * width), lambda i: (i, 0)),
        out_shape=jax.ShapeDtypeStruct((rows, 16 * width), BF),
        compiler_params=pltpu.CompilerParams(vmem_limit_bytes=4 << 20),
        name="merge",
    )(kept1, kept2, got1, got2)


def at(y, x, core):
    return (y % 4 * 4 + x % 4) * 2 + core


GROUPS = [[at(y, x, 0) for y in range(4)] for x in range(4)] + [
    [at(y, x, 1) for x in range(4)] for y in range(4)
]


def ring(shift):
    pairs = []
    for y in range(4):
        for x in range(4):
            pairs.append((at(y, x, 0), at(y, x + shift, 0)))
            pairs.append((at(y, x, 1), at(y + shift, x, 1)))
    return pairs


SWAP = [(d, d ^ 1) for d in range(32)]


def sent_to_all(value, axis, length, groups=None):
    return lax.all_to_all(
        jnp.broadcast_to(value[None], (length, *value.shape)),
        axis,
        0,
        0,
        tiled=True,
        axis_index_groups=groups,
    )


def moved(value, pairs):
    return lax.ppermute(value, "dp", pairs)


def per_device(up_pre, mix_pre, ln_gain, mix_weight, mix_bias, out_weight):
    slab = lax.all_gather(out_weight.T, "sp")
    own = sent_to_all(slab, "dp", 4, GROUPS)
    before = moved(own, ring(1))
    high1 = moved(own[:, 8:], ring(-1))
    low1 = moved(own[:, :8], ring(-1))
    normed = norm(mix_pre[0], ln_gain[None])
    gated = gate(normed, up_pre[0], mix_weight, mix_bias)
    high1, gated = lax.optimization_barrier((high1, gated))
    high2 = moved(high1, ring(-1))
    low2 = moved(before[:, :8], ring(1))
    partner = moved(gated, SWAP)
    kept1, sent1 = project(gated, partner, [(own,), (low1, high1), (before,)])
    got1 = moved(sent1, SWAP)
    low2, high2, kept1 = lax.optimization_barrier((low2, high2, kept1))
    kept2, sent2 = project(gated, partner, [(low2, high2)])
    got2 = moved(sent2, SWAP)
    return merge(kept1, kept2, got1, got2)[None]


def solution(mesh):
    return jax.shard_map(
        per_device,
        mesh=mesh,
        in_specs=(P("dp", "sp", None), P("dp", "sp", None), P(), P(), P(), P("sp", "dp")),
        out_specs=P("dp", "sp", None),
        check_vma=False,
    )
```

```python
import functools

import jax
import jax.numpy as jnp
from jax import lax
from jax.experimental import pallas as pl
from jax.experimental.pallas import tpu as pltpu
from jax.sharding import PartitionSpec as P


BLOCK = 128
norm_epsilon = 1e-05
HALF_ROOT = 0.7071067811865476
BF = jnp.bfloat16
F32 = jnp.float32


def gelu(x):
    return (0.5 * x) * (1.0 + lax.erf(x * HALF_ROOT))


def norm_kernel(mix_ref, gain_ref, out_ref, act_ref):
    rows, width = mix_ref.shape
    step = 16

    def body(i, _):
        at = pl.ds(pl.multiple_of(i * step, step), step)
        act = gelu(mix_ref[at, :].astype(F32))
        act_ref[at, :] = act
        center = jnp.sum(act, axis=-1, keepdims=True) * (1.0 / width)
        off = act - center
        spread = jnp.sum(off * off, axis=-1, keepdims=True) * (1.0 / width)
        scale = lax.rsqrt(spread + norm_epsilon)
        out_ref[at, :] = ((act_ref[at, :] - center) * scale * gain_ref[...]).astype(BF)
        return 0

    lax.fori_loop(0, rows // step, body, 0, unroll=2)


def norm(mix, gain):
    rows, width = mix.shape
    return pl.pallas_call(
        norm_kernel,
        grid=(rows // BLOCK,),
        in_specs=[
            pl.BlockSpec((BLOCK, width), lambda i: (i, 0)),
            pl.BlockSpec((1, width), lambda i: (0, 0)),
        ],
        out_specs=pl.BlockSpec((BLOCK, width), lambda i: (i, 0)),
        out_shape=jax.ShapeDtypeStruct((rows, width), BF),
        scratch_shapes=[pltpu.VMEM((BLOCK, width), F32)],
        compiler_params=pltpu.CompilerParams(vmem_limit_bytes=8 << 20),
        cost_estimate=pl.CostEstimate(
            flops=4_000_000_000, bytes_accessed=rows * width * 4, transcendentals=rows * width
        ),
        name="norm",
    )(mix, gain)


def gate_kernel(normed_ref, up_ref, weight_ref, bias_ref, out_ref):
    groups, block, _ = weight_ref.shape
    width = up_ref.shape[1] // groups
    keep = lax.broadcasted_iota(jnp.int32, (block, block), 0) >= lax.broadcasted_iota(
        jnp.int32, (block, block), 1
    )
    bias = jnp.transpose(bias_ref[...])
    for g in range(groups):
        cols = slice(g * width, (g + 1) * width)
        masked = jnp.where(keep, weight_ref[g].astype(F32), 0.0).astype(BF)
        mixed = jnp.dot(masked, normed_ref[:, cols], preferred_element_type=F32)
        mixed = mixed + bias[:, g : g + 1]
        up = gelu(up_ref[:, cols].astype(F32)).astype(BF).astype(F32)
        out_ref[:, cols] = (up * mixed).astype(BF)


def gate(normed, up, weight, bias):
    rows, width = up.shape
    groups = weight.shape[0]
    return pl.pallas_call(
        gate_kernel,
        grid=(rows // BLOCK,),
        in_specs=[
            pl.BlockSpec((BLOCK, width), lambda i: (i, 0)),
            pl.BlockSpec((BLOCK, width), lambda i: (i, 0)),
            pl.BlockSpec((groups, BLOCK, BLOCK), lambda i: (0, 0, 0)),
            pl.BlockSpec((groups, BLOCK), lambda i: (0, 0)),
        ],
        out_specs=pl.BlockSpec((BLOCK, width), lambda i: (i, 0)),
        out_shape=jax.ShapeDtypeStruct((rows, width), BF),
        compiler_params=pltpu.CompilerParams(vmem_limit_bytes=8 << 20),
        cost_estimate=pl.CostEstimate(
            flops=4_000_000_000, bytes_accessed=rows * width * 6, transcendentals=rows * width
        ),
        name="gate",
    )(normed, up, weight, bias)


def project_kernel(split, mine_ref, partner_ref, *refs):
    parts, kept_ref, sent_ref = refs[:-2], refs[-2], refs[-1]
    core = lax.axis_index("dp") & 1
    for n, (start, stop) in enumerate(zip(split, split[1:])):
        piece = parts[start:stop]
        count, blocks, width, _ = piece[0].shape
        rhs = jnp.concatenate(
            [
                jnp.concatenate([p[j, k] for p in piece for k in range(blocks)], axis=1)
                for j in range(count)
            ],
            axis=0,
        )
        for rows_ref, out_ref in ((mine_ref, kept_ref), (partner_ref, sent_ref)):
            result = lax.dot_general(
                rows_ref[...], rhs, (((1,), (1,)), ((), ())), preferred_element_type=F32
            )
            for m in range(count // 2):
                tile = result[:, m * 2 * width : (m + 1) * 2 * width]
                first = n * count + 2 * m
                out_ref[first + core] = tile.astype(BF)
                out_ref[first + 1 - core] = pltpu.roll(tile, width, 1).astype(BF)


def project(mine, partner, pieces):
    rows = mine.shape[0]
    count, _, width, _ = pieces[0][0].shape
    tiles = len(pieces) * count
    parts = [part for piece in pieces for part in piece]
    split = [sum(len(piece) for piece in pieces[:n]) for n in range(len(pieces) + 1)]
    vmem = pl.BlockSpec(memory_space=pltpu.VMEM)
    out = jax.ShapeDtypeStruct((tiles, rows, 2 * width), BF)
    return pl.pallas_call(
        functools.partial(project_kernel, split),
        in_specs=[vmem] * (2 + len(parts)),
        out_specs=[vmem, vmem],
        out_shape=[out, out],
        compiler_params=pltpu.CompilerParams(vmem_limit_bytes=6 << 20),
        cost_estimate=pl.CostEstimate(
            flops=4 * rows * width * tiles * mine.shape[1], bytes_accessed=4 << 20, transcendentals=0
        ),
        name="project",
    )(mine, partner, *parts)


ORDER = (0, 1, 3, 2)


def merge_kernel(kept1, kept2, got1, got2, out_ref):
    index = lax.axis_index("dp")
    core, x, y = index & 1, (index >> 1) & 3, index >> 3
    first, second = lax.select(core == 0, x, y), lax.select(core == 0, y, x)
    step = out_ref.shape[0]
    width = kept1.shape[2]
    rows = pl.ds(pl.multiple_of(pl.program_id(0) * step, step), step)
    lane = lax.broadcasted_iota(jnp.int32, (step, width), 1)
    ours = (lane // (width // 2)) == core

    def tile(refs, r, j):
        place = ORDER.index(r)
        return refs[0][place * 4 + j, rows, :] if place < 3 else refs[1][j, rows, :]

    for r in range(4):
        a = lax.rem(first + r, 4)
        for t in range(4):
            b = lax.rem(second + t, 4)
            at = lax.select(core == 0, b * 4 + a, a * 4 + b)
            kept = tile((kept1, kept2), r, b)
            got = tile((got1, got2), t, a)
            where = pl.ds(pl.multiple_of(at * width, width), width)
            out_ref[:, where] = jnp.where(ours, kept, got)


def merge(kept1, kept2, got1, got2):
    rows, width = kept1.shape[1:]
    vmem = pl.BlockSpec(memory_space=pltpu.VMEM)
    return pl.pallas_call(
        merge_kernel,
        grid=(rows // BLOCK,),
        in_specs=[vmem] * 4,
        out_specs=pl.BlockSpec((BLOCK, 16 * width), lambda i: (i, 0)),
        out_shape=jax.ShapeDtypeStruct((rows, 16 * width), BF),
        compiler_params=pltpu.CompilerParams(vmem_limit_bytes=4 << 20),
        name="merge",
    )(kept1, kept2, got1, got2)


def at(y, x, core):
    return (y % 4 * 4 + x % 4) * 2 + core


GROUPS = [[at(y, x, 0) for y in range(4)] for x in range(4)] + [
    [at(y, x, 1) for x in range(4)] for y in range(4)
]


def ring(shift):
    pairs = []
    for y in range(4):
        for x in range(4):
            pairs.append((at(y, x, 0), at(y, x + shift, 0)))
            pairs.append((at(y, x, 1), at(y + shift, x, 1)))
    return pairs


SWAP = [(d, d ^ 1) for d in range(32)]


def sent_to_all(value, axis, length, groups=None):
    return lax.all_to_all(
        jnp.broadcast_to(value[None], (length, *value.shape)),
        axis,
        0,
        0,
        tiled=True,
        axis_index_groups=groups,
    )


def moved(value, pairs):
    return lax.ppermute(value, "dp", pairs)


def per_device(up_pre, mix_pre, ln_gain, mix_weight, mix_bias, out_weight):
    slab = sent_to_all(out_weight.T, "sp", 16)
    normed = norm(mix_pre[0], ln_gain[None])
    gated = gate(normed, up_pre[0], mix_weight, mix_bias)
    partner = moved(gated, SWAP)
    slab, partner = lax.optimization_barrier((slab, partner))
    own = sent_to_all(slab, "dp", 4, GROUPS)
    low3 = moved(own[:, :8], ring(1))
    high1 = moved(own[:, 8:], ring(-1))
    high3 = moved(own[:, 8:], ring(1))
    low1 = moved(own[:, :8], ring(-1))
    low2 = moved(low3, ring(1))
    high2 = moved(high1, ring(-1))
    kept1, sent1 = project(gated, partner, [(own,), (low1, high1), (low3, high3)])
    got1 = moved(sent1, SWAP)
    low2, high2, kept1 = lax.optimization_barrier((low2, high2, kept1))
    kept2, sent2 = project(gated, partner, [(low2, high2)])
    got2 = moved(sent2, SWAP)
    return merge(kept1, kept2, got1, got2)[None]


def solution(mesh):
    return jax.shard_map(
        per_device,
        mesh=mesh,
        in_specs=(P("dp", "sp", None), P("dp", "sp", None), P(), P(), P(), P("sp", "dp")),
        out_specs=P("dp", "sp", None),
        check_vma=False,
    )
```
